256 devices in a mesh: sp: 32 (over z, x), fs: 4 (over y), tp: 2 (over core).
Axes of the slice: x: 4, y: 4, z: 8, core: 2. Of those that a mesh axis runs over, the one named last changes fastest.
Arguments:
- inputs: bfloat16 [4, 4096, 2048], P('fs', 'sp', 'tp'), may hold values from -6 to 6
- input_norm_scale: float32 [2048], replicated, may hold values from 0.1 to 1.9
- query_matrix: bfloat16 [2048, 512], P('sp', 'tp'), may hold values from -0.125 to 0.125
- key_matrix: bfloat16 [2048, 512], P('sp', 'tp'), may hold values from -0.125 to 0.125
- value_matrix: bfloat16 [2048, 512], P('sp', 'tp'), may hold values from -0.125 to 0.125
- decay_down_weight: bfloat16 [2048, 128], replicated, may hold values from -0.125 to 0.125
- decay_up_weight: bfloat16 [128, 512], P(None, 'tp'), may hold values from -1.1953125 to 1.1953125
- decay_bias_base: float32 [512], P('tp'), as said below
- decay_position_offset: float32 [4, 4096, 8], P('fs', 'sp', 'tp'), may hold values from -0.7 to 0.7
- extra_log_decay: float32 [4, 4096, 8], P('fs', 'sp', 'tp'), may hold values from -2.8 to 0, as said below
- correction_down_weight: bfloat16 [2048, 128], replicated, may hold values from -0.125 to 0.125
- correction_up_weight: bfloat16 [128, 512], P(None, 'tp'), may hold values from -1.1953125 to 1.1953125
- correction_rate_bias: float32 [512], P('tp'), as said below
- head_norm_scale: float32 [512], P('tp'), may hold values from 0.1 to 1.9
- starting_states: float32 [4, 2, 8, 64, 64], P('fs', None, 'tp'), may hold values from -384 to 384
- pointwise_value_weight: bfloat16 [2048, 1024], P('sp', 'tp'), may hold values from -0.125 to 0.125
- pointwise_gate_weight: bfloat16 [2048, 1024], P('sp', 'tp'), may hold values from -0.125 to 0.125
- depthwise_taps_weight: float32 [31, 1024], P(None, 'tp')
- channel_norm_scale: float32 [1024], P('tp'), may hold values from 0.1 to 1.9
- mixer_output_weight: bfloat16 [512, 2048], P('tp', 'sp'), may hold values from -0.15625 to 0.15625
- convolution_output_weight: bfloat16 [1024, 2048], P('tp', 'sp'), may hold values from -0.15625 to 0.15625
Outputs:
- mixed: bfloat16 [4, 4096, 2048], P('fs', ('sp', 'tp'))
The draws below stay inside these ranges and needn't reach their ends.
Inputs may be any that keep to these rules, and one draw needn't show every extreme that they name: `decay_bias_base`: decay bases, one value for every channel. `correction_rate_bias`: correction-rate bases, one value for every channel. `extra_log_decay`: zero at all but a few positions of each sequence.
All inputs are finite; a program needn't handle non-finite values.
Results may differ from the reference program's by a relative error of at most 0.012.
Values may be sent and summed in bfloat16 or wider, within the bound.
No kernel may reach another device: no remote copies, remote signals or barrier semaphores. Data moves between devices by JAX's collectives and lax.ppermute only.
A program may use at most 64 MiB of HBM per device.

```python
import jax
import jax.numpy as jnp
from jax import lax

D = 2048
ATTN_GROUP_SIZE = 64
RANK = 128
CONV_K = 31
RW_H = 8
TOK_DEV = 128
RW_W = 512
CW = 1024
SEQ_LEN = 4096
BATCH = 4


def slow_heads(key):
    order = jax.random.permutation(jax.random.fold_in(key, 11), RW_H)
    return order >= RW_H // 2


def draw_decay_bias_base(key, part):
    slow = jnp.repeat(slow_heads(key), ATTN_GROUP_SIZE)
    jitter = jax.random.uniform(jax.random.fold_in(key, 12), (RW_H * ATTN_GROUP_SIZE,), jnp.float32, -0.5, 0.5)
    slow_value = jnp.log(0.25 / SEQ_LEN) + 0.5
    return jnp.where(slow, slow_value, -3.0) + jitter


def draw_correction_rate_bias(key, part):
    slow = jnp.repeat(slow_heads(key), ATTN_GROUP_SIZE)
    jitter = jax.random.uniform(jax.random.fold_in(key, 13), (RW_H * ATTN_GROUP_SIZE,), jnp.float32, -0.5, 0.5)
    spread = jax.random.uniform(jax.random.fold_in(key, 14), (RW_H * ATTN_GROUP_SIZE,), jnp.float32, -1.0, 1.0)
    return jnp.where(slow, jnp.log(16.0 / SEQ_LEN) + jitter, spread)


def draw_decay_position_offset(key, part):
    blocks = SEQ_LEN // TOK_DEV
    offsets = jax.random.uniform(jax.random.fold_in(key, 15), (BATCH, blocks, RW_H), jnp.float32, -0.7, 0.7)
    return jnp.repeat(offsets, TOK_DEV, axis=1)


def draw_extra_log_decay(key, part):
    places = jax.random.randint(jax.random.fold_in(key, 21), (BATCH, 4), 0, SEQ_LEN)
    losses = jnp.log(jax.random.uniform(jax.random.fold_in(key, 22), (BATCH, 4, RW_H), jnp.float32, 0.5, 0.8))
    hits = (jnp.arange(SEQ_LEN)[None, :, None] == places[:, None, :]).astype(jnp.float32)
    return jnp.einsum('blp,bph->blh', hits, losses)


def draw_depthwise_taps_weight(key, part):
    rising = jnp.exp(jnp.linspace(jnp.log(0.3), jnp.log(3.0), CW))
    values = jax.random.normal(jax.random.fold_in(key, 23), (CONV_K, CW), jnp.float32)
    return values * rising[None, :] / jnp.sqrt(float(CONV_K))


def level_of(rng, dims, shards, smallest, largest):
    loudness = 1.0
    for axis_at, parts in shards:
        draws = jax.random.uniform(jax.random.fold_in(jax.random.fold_in(rng, 6), axis_at), (parts,), jnp.float32, smallest / len(shards), largest / len(shards))
        loudness = loudness * jnp.repeat(jnp.exp(draws), dims[axis_at] // parts).reshape((-1,) + (1,) * (len(dims) - 1 - axis_at))
    return loudness


def normal_values(own_key, extent, scale, most, split=(), kind=jnp.bfloat16):
    result = jax.random.normal(own_key, extent, jnp.float32) * scale
    if len(split) > 0:
        result = level_of(own_key, extent, split, -0.22, 0.18) * result
    return jnp.clip(result, min=-most, max=most).astype(kind)


def setup_inputs(seed: int = 0) -> dict:
    streams_of = jax.random.split(jax.random.key(seed), 22)
    inputs = normal_values(streams_of[0], (BATCH, SEQ_LEN, D), 1.0, 6.0, ((0, 4), (1, 32), (2, 2)))
    input_norm_scale = jnp.clip(1.0 + 0.18 * jax.random.normal(streams_of[1], (D,), jnp.float32), 0.1, 1.9)
    query_matrix = normal_values(streams_of[2], (D, RW_W), D ** -0.5, 0.125, ((0, 32), (1, 2)))
    key_matrix = normal_values(streams_of[3], (D, RW_W), D ** -0.5, 0.125, ((0, 32), (1, 2)))
    value_matrix = normal_values(streams_of[4], (D, RW_W), D ** -0.5, 0.125, ((0, 32), (1, 2)))
    decay_down_weight = normal_values(streams_of[5], (D, RANK), D ** -0.5, 0.125)
    decay_up_weight = normal_values(streams_of[6], (RANK, RW_W), 0.2, 1.1953125, ((1, 2),))
    decay_bias_base = draw_decay_bias_base(jax.random.fold_in(streams_of[21], 71), 0)
    decay_position_offset = draw_decay_position_offset(jax.random.fold_in(streams_of[21], 71), 0)
    extra_log_decay = draw_extra_log_decay(jax.random.fold_in(streams_of[21], 71), 0)
    correction_down_weight = normal_values(streams_of[10], (D, RANK), D ** -0.5, 0.125)
    correction_up_weight = normal_values(streams_of[11], (RANK, RW_W), 0.2, 1.1953125, ((1, 2),))
    correction_rate_bias = draw_correction_rate_bias(jax.random.fold_in(streams_of[21], 71), 0)
    head_norm_scale = jnp.clip(1.0 + 0.18 * jax.random.normal(streams_of[13], (RW_W,), jnp.float32), 0.1, 1.9)
    starting_states = normal_values(streams_of[14], (BATCH, 2, RW_H, ATTN_GROUP_SIZE, ATTN_GROUP_SIZE), (SEQ_LEN ** 0.5), 384.0, ((0, 4), (2, 2)), jnp.float32)
    pointwise_value_weight = normal_values(streams_of[15], (D, CW), D ** -0.5, 0.125, ((0, 32), (1, 2)))
    pointwise_gate_weight = normal_values(streams_of[16], (D, CW), D ** -0.5, 0.125, ((0, 32), (1, 2)))
    depthwise_taps_weight = draw_depthwise_taps_weight(jax.random.fold_in(streams_of[21], 71), 0)
    channel_norm_scale = jnp.clip(1.0 + 0.18 * jax.random.normal(streams_of[18], (CW,), jnp.float32), 0.1, 1.9)
    mixer_output_weight = normal_values(streams_of[19], (RW_W, D), (RW_W + CW) ** -0.5, 0.15625, ((0, 2), (1, 32)))
    convolution_output_weight = normal_values(streams_of[20], (CW, D), (RW_W + CW) ** -0.5, 0.15625, ((0, 2), (1, 32)))
    return dict(inputs=inputs, input_norm_scale=input_norm_scale, query_matrix=query_matrix, key_matrix=key_matrix, value_matrix=value_matrix, decay_down_weight=decay_down_weight, decay_up_weight=decay_up_weight, decay_bias_base=decay_bias_base, decay_position_offset=decay_position_offset, extra_log_decay=extra_log_decay, correction_down_weight=correction_down_weight, correction_up_weight=correction_up_weight, correction_rate_bias=correction_rate_bias, head_norm_scale=head_norm_scale, starting_states=starting_states, pointwise_value_weight=pointwise_value_weight, pointwise_gate_weight=pointwise_gate_weight, depthwise_taps_weight=depthwise_taps_weight, channel_norm_scale=channel_norm_scale, mixer_output_weight=mixer_output_weight, convolution_output_weight=convolution_output_weight)


highest = lax.Precision.HIGHEST

def split_heads(values):
    return values.reshape(values.shape[0], -1, ATTN_GROUP_SIZE)

def paired(values):
    return jnp.stack([values, jnp.flip(values, 0)], 1)

def state_step(state, inputs):
    fading_multiplier, unit_key, rated_key, keys, values, query = inputs
    projected = jnp.einsum('dhvk,dhk->dhv', state, unit_key, precision=highest)
    state = state * fading_multiplier[:, :, None, :] - projected[..., None] * rated_key[:, :, None, :] + values[..., None] * keys[:, :, None, :]
    return (state, jnp.einsum('dhvk,dhk->dhv', state, query, precision=highest))

def head_norm(summed, head_norm_scale):
    centered = summed - lax.optimization_barrier(jnp.mean(summed, axis=-1, keepdims=True))
    scaled = centered * lax.rsqrt(lax.optimization_barrier(jnp.mean(centered * centered, axis=-1, keepdims=True)) + 0.00064)
    return (scaled * head_norm_scale.reshape(-1, ATTN_GROUP_SIZE)).reshape(summed.shape[0], -1).astype(jnp.bfloat16)

def reference(inputs, input_norm_scale, query_matrix, key_matrix, value_matrix, decay_down_weight, decay_up_weight, decay_bias_base, decay_position_offset, extra_log_decay, correction_down_weight, correction_up_weight, correction_rate_bias, head_norm_scale, starting_states, pointwise_value_weight, pointwise_gate_weight, depthwise_taps_weight, channel_norm_scale, mixer_output_weight, convolution_output_weight):

    def single_sequence(entry_collection):
        symbol_vectors, location_shift, fading_spike_amount, initial_memory_matrix = entry_collection
        as_float = symbol_vectors.astype(jnp.float32)
        normed = (as_float * lax.rsqrt(lax.optimization_barrier(jnp.mean(as_float * as_float, axis=-1, keepdims=True)) + 1e-06) * input_norm_scale).astype(jnp.bfloat16)

        def project(weight):
            return jnp.dot(normed, weight, preferred_element_type=jnp.float32)

        def rounded(total):
            return lax.optimization_barrier(total.astype(jnp.bfloat16)).astype(jnp.float32)
        query = rounded(project(query_matrix))
        keys = rounded(project(key_matrix))
        values = rounded(project(value_matrix))
        low_decay = jnp.tanh(project(decay_down_weight)).astype(jnp.bfloat16)
        fading_raw_scores = decay_bias_base + jnp.dot(low_decay, decay_up_weight, preferred_element_type=jnp.float32) + jnp.repeat(location_shift, ATTN_GROUP_SIZE, axis=1)
        fading_multiplier = jnp.exp(-jnp.exp(-jax.nn.softplus(-fading_raw_scores) - 0.5) + jnp.repeat(fading_spike_amount, ATTN_GROUP_SIZE, axis=1))
        low_rate = project(correction_down_weight).astype(jnp.bfloat16)
        rate = jax.nn.sigmoid(correction_rate_bias + jnp.dot(low_rate, correction_up_weight, preferred_element_type=jnp.float32))
        key_heads = split_heads(keys)
        unit_key = key_heads * lax.rsqrt(lax.optimization_barrier(jnp.sum(key_heads * key_heads, axis=-1, keepdims=True)) + 1e-06)
        rated_key = unit_key * split_heads(rate)
        steps = tuple((paired(item) for item in (split_heads(fading_multiplier), unit_key, rated_key, key_heads, split_heads(values), split_heads(query))))
        final, outputs = lax.scan(state_step, initial_memory_matrix, steps)
        summed = outputs[:, 0] + jnp.flip(outputs[:, 1], 0)
        mixer_out = head_norm(summed, head_norm_scale)
        glu = (project(pointwise_value_weight) * jax.nn.sigmoid(project(pointwise_gate_weight))).astype(jnp.bfloat16)
        reach = depthwise_taps_weight.shape[0] // 2
        padded = jnp.pad(glu.astype(jnp.float32), ((reach, reach), (0, 0)))
        conv = lax.conv_general_dilated(padded[None], depthwise_taps_weight[:, None, :], (1,), 'VALID', dimension_numbers=('NWC', 'WIO', 'NWC'), feature_group_count=depthwise_taps_weight.shape[1], precision=highest)[0]
        width = conv.shape[1]
        mean = lax.optimization_barrier(jnp.sum(conv, axis=-1)) / width
        power = lax.optimization_barrier(jnp.sum(conv * conv, axis=-1)) / width - mean * mean
        conv_out = jax.nn.silu((conv - mean[:, None]) * lax.rsqrt(power[:, None] + 1e-05) * channel_norm_scale).astype(jnp.bfloat16)
        total = jnp.dot(mixer_out, mixer_output_weight, preferred_element_type=jnp.float32) + jnp.dot(conv_out, convolution_output_weight, preferred_element_type=jnp.float32)
        return total.astype(jnp.bfloat16)
    return lax.map(single_sequence, (inputs, decay_position_offset, extra_log_decay, starting_states))
```

```python
import jax
import jax.numpy as jnp
from jax import lax
from jax.experimental import pallas as pl
from jax.experimental.pallas import tpu as pltpu
from jax.sharding import Mesh
from jax.sharding import PartitionSpec as P

BF = jnp.bfloat16
F32 = jnp.float32
CH = 64
ROWS = 512
GRP = 256
VM = pl.BlockSpec(memory_space=pltpu.VMEM)
SM = pl.BlockSpec(memory_space=pltpu.SMEM)


def call(body, outs, n_smem, n_vmem, scratch=(), flops=0, name=None):
    return pl.pallas_call(
        body,
        out_shape=[jax.ShapeDtypeStruct(s, d) for s, d in outs],
        in_specs=[SM] * n_smem + [VM] * n_vmem,
        out_specs=[VM] * len(outs),
        scratch_shapes=list(scratch),
        cost_estimate=pl.CostEstimate(flops=flops, bytes_accessed=0, transcendentals=0),
        name=name,
    )


def dot(a, b):
    return jnp.dot(a, b, preferred_element_type=F32)


def dot_nt(a, b):
    return lax.dot_general(a, b, (((1,), (1,)), ((), ())), preferred_element_type=F32)


def dot_tn(a, b, precision=None):
    return lax.dot_general(
        a, b, (((0,), (0,)), ((), ())), preferred_element_type=F32, precision=precision
    )


def low_lanes(shape):
    return lax.broadcasted_iota(jnp.int32, shape, len(shape) - 1) < CH


def half_roll(v):
    return pltpu.roll(v, CH, v.ndim - 1)


SHIFTS = (0, 1, -1, 2)


def prepare_body(
    idx, a0, a1, a2, a3, p0, p1, p2, p3, m0, m1, m2, m3, scale, ddw, cdw, dup, cup, db, cb,
    normed, pu, pr, pq, rate, pos, spike,
):
    x, c = idx[1], idx[3]
    mine = pl.multiple_of(c * 1024, 1024)
    other = pl.multiple_of((1 - c) * 1024, 1024)
    row8 = lax.broadcasted_iota(jnp.int32, (8, 128), 0)
    pick_pos = (row8 == x).astype(F32)
    pick_spike = (row8 == x + 4).astype(F32)
    for shift, a, p, m in zip(SHIFTS, (a0, a1, a2, a3), (p0, p1, p2, p3), (m0, m1, m2, m3)):
        row0 = pl.multiple_of(lax.rem(x - shift + 4, 4) * 128, 128)

        def rows(i, carry, a=a, p=p, row0=row0):
            r = pl.ds(pl.multiple_of(i * 16, 16), 16)
            to = pl.ds(pl.multiple_of(row0 + i * 16, 16), 16)
            own = a[r, :].astype(F32)
            far = p[r, :].astype(F32)
            power = jnp.sum(own * own, axis=1, keepdims=True) + jnp.sum(
                far * far, axis=1, keepdims=True
            )
            inv = lax.rsqrt(power * (1.0 / 2048) + 1e-6)
            normed[to, pl.ds(mine, 1024)] = (own * inv * scale[pl.ds(c, 1), :]).astype(BF)
            normed[to, pl.ds(other, 1024)] = (far * inv * scale[pl.ds(1 - c, 1), :]).astype(BF)
            return carry

        lax.fori_loop(0, 8, rows, 0)
        block = m[...]
        pos[pl.ds(row0, 128), :] = dot_tn(block, pick_pos, lax.Precision.HIGHEST)
        spike[pl.ds(row0, 128), :] = dot_tn(block, pick_spike, lax.Precision.HIGHEST)
    low = dot(normed[...], jnp.concatenate([ddw[...], cdw[...]], axis=1))
    low_decay = jnp.tanh(low[:, :128]).astype(BF)
    low_rate = low[:, 128:].astype(BF)
    pre = db[...] + dot(low_decay, dup[...]) + pos[...]
    logd = spike[...] - jax.nn.sigmoid(pre) * 0.6065306597126334
    rate[...] = jax.nn.sigmoid(cb[...] + dot(low_rate, cup[...]))
    lo = low_lanes((ROWS, 128))
    head = logd.astype(BF)
    tail = (logd - head.astype(F32)).astype(BF)
    parts = jnp.where(lo, head, tail)
    t = lax.broadcasted_iota(jnp.int32, (GRP, GRP), 0)
    s = lax.broadcasted_iota(jnp.int32, (GRP, GRP), 1)
    same = t // CH == s // CH
    mid = (s // CH) * CH + CH // 2
    sign = jnp.where(same & (s >= mid) & (s < t), 1.0, 0.0) - jnp.where(
        same & (s < mid) & (s >= t), 1.0, 0.0
    )
    sign = sign.astype(BF)
    both = jnp.concatenate([dot(sign, parts[:GRP]), dot(sign, parts[GRP:])], axis=0)
    before = both + half_roll(both)
    upto = before + logd
    pu[...] = jnp.exp(jnp.where(lo, before, -upto))
    pr[...] = jnp.exp(jnp.where(lo, -upto, before))
    pq[...] = jnp.exp(jnp.where(lo, upto, -before))


def prepare(*args):
    full = ((ROWS, 128), F32)
    return call(
        prepare_body,
        [((ROWS, 2048), BF), full, full, full, full],
        1,
        19,
        [pltpu.VMEM((ROWS, 128), F32), pltpu.VMEM((ROWS, 128), F32)],
        flops=2 * ROWS * 2048 * 256,
        name="prepare",
    )(*args)


def chunk_gain(pq, j):
    top = pq[pl.ds(j * CH, 1), :]
    bottom = pq[pl.ds(j * CH + CH - 1, 1), :]
    return jnp.where(low_lanes((1, 128)), bottom, top)


def maps_body(idx, normed, wkv, pu, pr, pq, rate, send, resp, rs_out, ks_out, kv_out, pre_out, xs, ta):
    kv = dot(normed[...], wkv[...]).astype(BF)
    kv_out[...] = kv
    kvf = kv.astype(F32)
    lo = low_lanes((ROWS, 128))
    turned = half_roll(kvf)
    kk = jnp.where(lo, kvf, turned)
    norm = lax.rsqrt(jnp.sum(kk * kk, axis=1, keepdims=True) * 0.5 + 1e-6)
    unit = kk * norm
    us = unit * pu[...]
    rsf = unit * rate[...] * pr[...]
    ksf = kk * pr[...]
    rs = rsf.astype(BF)
    ks = ksf.astype(BF)
    rs_out[...] = rs
    ks_out[...] = ks
    zero = jnp.zeros((), F32)
    v_high = jnp.where(lo, zero, kvf).astype(BF)
    v_low = jnp.where(lo, turned, zero).astype(BF)
    gains = [chunk_gain(pq, j) for j in range(8)]
    starts = [half_roll(g) for g in gains]

    t = lax.broadcasted_iota(jnp.int32, (GRP, GRP), 0)
    s = lax.broadcasted_iota(jnp.int32, (GRP, GRP), 1)
    same = t // CH == s // CH
    fine = t // 16 == s // 16
    lane = lax.broadcasted_iota(jnp.int32, (16, 128), 1)
    sub = lax.broadcasted_iota(jnp.int32, (16, 128), 0)
    eye16 = (lane % 16 == sub).astype(F32)

    rhs_all, n_all, packed = [], [], []
    for back in (False, True):
        u_dir = jnp.where(lo, zero, us) if back else jnp.where(lo, us, zero)
        ub = u_dir.astype(BF)
        strict = same & ((s > t) if back else (s < t))
        for g in range(2):
            rows = slice(g * GRP, g * GRP + GRP)
            n = jnp.where(strict, dot_nt(ub[rows], rs[rows]), zero)
            a = jnp.where(strict, dot_nt(ub[rows], ks[rows]), zero).astype(BF)
            first = jnp.concatenate(
                [u_dir[g * GRP + q * CH : g * GRP + q * CH + CH] * starts[g * 4 + q] for q in range(4)],
                axis=0,
            )
            rhs = first + dot(a, (v_low if back else v_high)[rows])
            rhs_all.append(rhs.astype(BF))
            n_all.append(jnp.where(fine, zero, n).astype(BF))
            for tile in range(2):
                acc = jnp.zeros((16, 128), F32)
                for i in range(8):
                    b = tile * 8 + i
                    acc = acc + jnp.where(
                        lane // 16 == i, n[b * 16 : b * 16 + 16, tile * 128 : tile * 128 + 128], zero
                    )
                packed.append(acc)
    solved = []
    for back in (False, True):
        tiles = packed[4 * back : 4 * back + 4]
        inv = [eye16] * 4
        for step in range(15):
            m = 15 - step if back else step
            where = (lane // 16) * 16 + m
            for k in range(4):
                coef = jnp.take_along_axis(tiles[k], where, axis=1)
                inv[k] = inv[k] - coef * inv[k][m : m + 1, :]
        solved += inv
    for i in range(4):
        back, g = divmod(i, 2)
        for b in range(16):
            tile = b // 8
            piece = jnp.where(lane // 16 == b % 8, solved[2 * i + tile], zero).astype(BF)
            empty = jnp.zeros((16, 128), BF)
            xs[b * 16 : b * 16 + 16, :] = jnp.concatenate(
                [piece, empty] if tile == 0 else [empty, piece], axis=1
            )
        xd = xs[...]
        y = dot(xd, rhs_all[i])
        z = dot(xd, n_all[i]).astype(BF)
        a = y - dot(z, y.astype(BF))
        p = a + dot(z, dot(z, a.astype(BF)).astype(BF))
        resp[back, g * GRP : g * GRP + GRP, :] = p.astype(BF)

    tt = lax.broadcasted_iota(jnp.int32, (128, 128), 0)
    ss = lax.broadcasted_iota(jnp.int32, (128, 128), 1)
    eye = tt == ss
    lo2 = ss < CH
    diag = (tt < CH) == lo2
    for j in range(8):
        rows = slice(j * CH, j * CH + CH)
        gain = gains[j]
        right = jnp.concatenate([ksf[rows] * gain, rsf[rows] * (-gain)], axis=0).astype(BF)
        through = gain * starts[j]
        f = dot_tn(jnp.concatenate([v_high[rows], resp[0, rows, :]], axis=0), right)
        b = dot_tn(jnp.concatenate([v_low[rows], resp[1, rows, :]], axis=0), right)
        keep = jnp.where(eye, through, zero)
        ta[0, j] = f + keep
        ta[1, j] = b + keep
    state = eye.astype(F32)
    for j in range(8):
        pre_out[j] = state.astype(BF)
        step = jnp.where(lo2, ta[0, j], ta[1, 7 - j])
        move = jnp.where(diag, step, zero)
        add = jnp.where(diag, zero, step)
        move_hi = move.astype(BF)
        move_lo = (move - move_hi.astype(F32)).astype(BF)
        st_hi = state.astype(BF)
        st_lo = (state - st_hi.astype(F32)).astype(BF)
        left = jnp.concatenate([st_hi, st_lo], axis=1)
        state = dot(left, jnp.concatenate([move_hi, move_hi], axis=0)) + dot(st_hi, move_lo) + add
    top, bottom = state[:CH], state[CH:]
    lo3 = low_lanes((CH, 128))
    forward = jnp.where(lo3, top, half_roll(bottom)).astype(BF)
    backward = jnp.where(lo3, half_roll(top), bottom).astype(BF)
    for d in range(8):
        send[d] = jnp.where(d > idx[0], forward, backward)


def maps(*args):
    full = ((ROWS, 128), BF)
    return call(
        maps_body,
        [((8, CH, 128), BF), ((2, ROWS, 128), BF), full, full, full, ((8, 128, 128), BF)],
        1,
        6,
        [pltpu.VMEM((GRP, GRP), BF), pltpu.VMEM((2, 8, 128, 128), F32)],
        flops=2 * ROWS * 2048 * 128 + 16 * 2 * 256**3,
        name="maps",
    )(*args)


def reads_body(normed, wq, pq, resp, rs, ks, kv, pre, thr_out, own_out):
    qq = dot(normed[...], wq[:, 0:128]).astype(BF).astype(F32)
    lo = low_lanes((ROWS, 128))
    zero = jnp.zeros((), F32)
    qs = qq * pq[...]
    kvf = kv[...].astype(F32)
    v_high = jnp.where(lo, zero, kvf).astype(BF)
    v_low = jnp.where(lo, half_roll(kvf), zero).astype(BF)
    t = lax.broadcasted_iota(jnp.int32, (GRP, GRP), 0)
    s = lax.broadcasted_iota(jnp.int32, (GRP, GRP), 1)
    same = t // CH == s // CH
    lo_c = low_lanes((CH, 128))
    full = [[], []]
    for back in (False, True):
        q_dir = jnp.where(lo, zero, qs) if back else jnp.where(lo, qs, zero)
        qb = q_dir.astype(BF)
        incl = same & ((s >= t) if back else (s <= t))
        v_dir = v_low if back else v_high
        for g in range(2):
            rows = slice(g * GRP, g * GRP + GRP)
            ar = jnp.where(incl, dot_nt(qb[rows], rs[rows, :]), zero).astype(BF)
            ak = jnp.where(incl, dot_nt(qb[rows], ks[rows, :]), zero).astype(BF)
            part = dot(ak, v_dir[rows]) - dot(ar, resp[int(back), rows, :])
            for c in range(4):
                j = g * 4 + c
                gain = half_roll(chunk_gain(pq, j))
                piece = part[c * CH : c * CH + CH]
                from_q = q_dir[j * CH : j * CH + CH] * gain
                keep = jnp.where(lo_c, zero, piece) if not back else jnp.where(lo_c, piece, zero)
                thr = (piece - keep + from_q).astype(BF)
                slot = 7 - j if back else j
                full[back].append(dot_nt(thr, pre[slot]) + keep)
    fwd = jnp.concatenate(full[0], axis=0)
    bwd = jnp.concatenate(full[1], axis=0)
    thr_out[...] = jnp.where(lo, fwd, bwd).astype(BF)
    own = jnp.where(lo, bwd, fwd)
    own_out[...] = own + half_roll(own)


def reads(*args):
    return call(
        reads_body,
        [((ROWS, 128), BF), ((ROWS, 128), F32)],
        0,
        8,
        flops=2 * ROWS * 2048 * 128 + 8 * 2 * 256**3,
        name="reads",
    )(*args)


def finish_body(idx, recv, s0, thr, own, scale, o0, o1, o2, o3, mixed):
    z, x = idx[0], idx[1]
    lo = low_lanes((CH, 128))
    state = s0[...]
    zero = jnp.zeros((), F32)
    for i in range(7):
        f = recv[i].astype(F32)
        b = recv[7 - i].astype(F32)
        move = jnp.concatenate([jnp.where(lo, f, zero), jnp.where(lo, zero, b)], axis=0).astype(BF)
        add = half_roll(jnp.where(lo, b, f))
        st_hi = state.astype(BF)
        st_lo = (state - st_hi.astype(F32)).astype(BF)
        new = dot(jnp.concatenate([st_hi, st_lo], axis=1), jnp.concatenate([move, move], axis=0)) + add
        use_f = i < z
        use_b = 7 - i > z
        use = jnp.where(lo, use_f.astype(jnp.int32), use_b.astype(jnp.int32)) > 0
        state = jnp.where(use, new, state)
    total = dot_nt(thr[...], state.astype(BF)) + own[:, :CH]
    centered = total - jnp.mean(total, axis=1, keepdims=True)
    scaled = centered * lax.rsqrt(jnp.mean(centered * centered, axis=1, keepdims=True) + 0.00064)
    mixed[...] = (scaled * scale[...]).astype(BF)
    for shift, o in zip(SHIFTS, (o0, o1, o2, o3)):
        row0 = pl.multiple_of(lax.rem(x + shift + 4, 4) * 128, 128)
        o[...] = mixed[pl.ds(row0, 128), :]


def finish(*args):
    return call(
        finish_body,
        [((128, CH), BF)] * 4,
        1,
        5,
        [pltpu.VMEM((ROWS, CH), BF)],
        flops=10**8,
        name="finish",
    )(*args)


def glu_body(normed, wg, glu, top, bottom):
    both = dot(normed[...], wg[:, 128:384])
    g = (both[:, :128] * jax.nn.sigmoid(both[:, 128:])).astype(BF)
    glu[...] = g
    top[...] = g[:16]
    bottom[...] = g[ROWS - 16 :]


def gated(*args):
    return call(
        glu_body,
        [((ROWS, 128), BF), ((16, 128), BF), ((16, 128), BF)],
        0,
        2,
        flops=2 * ROWS * 2048 * 256,
        name="gated",
    )(*args)


def conv_body(idx, glu, low, high, taps, o0, o1, o2, o3, pad, out):
    x = idx[1]
    pad[0:16, :] = low[...].astype(F32)
    pad[16 : 16 + ROWS, :] = glu[...].astype(F32)
    pad[16 + ROWS : 32 + ROWS, :] = high[...].astype(F32)

    def tile(i, carry):
        base = pl.multiple_of(i * 64, 64)
        acc = jnp.zeros((64, 128), F32)
        for j in range(31):
            acc = acc + taps[j : j + 1, :] * pad[pl.ds(base + j + 1, 64), :]
        out[pl.ds(base, 64), :] = acc.astype(BF)
        return carry

    lax.fori_loop(0, ROWS // 64, tile, 0)
    for shift, o in zip(SHIFTS, (o0, o1, o2, o3)):
        row0 = pl.multiple_of(lax.rem(x + shift + 4, 4) * 128, 128)
        o[...] = out[pl.ds(row0, 128), :]


def conv(*args):
    return call(
        conv_body,
        [((128, 128), BF)] * 4,
        1,
        4,
        [pltpu.VMEM((ROWS + 32, 128), F32), pltpu.VMEM((ROWS, 128), BF)],
        flops=2 * ROWS * 128 * 31 * 8,
        name="conv",
    )(*args)


def stats_body(idx, c0, c1, c2, c3, joined, stat):
    x = idx[1]
    first = jnp.zeros((128, 1), F32)
    second = jnp.zeros((128, 1), F32)
    for shift, ref in zip(SHIFTS, (c0, c1, c2, c3)):
        at = pl.multiple_of(lax.rem(x - shift + 4, 4) * 128, 128)
        block = ref[...]
        joined[:, pl.ds(at, 128)] = block
        wide = block.astype(F32)
        first = first + jnp.sum(wide, axis=1, keepdims=True)
        second = second + jnp.sum(wide * wide, axis=1, keepdims=True)
    lane = lax.broadcasted_iota(jnp.int32, (128, 128), 1)
    stat[...] = jnp.where(lane == 0, first, second)


def stats(*args):
    return call(
        stats_body, [((128, 512), BF), ((128, 128), F32)], 1, 4, flops=10**6, name="stats"
    )(*args)


def assemble_body(idx, w0, w1, w2, w3, out):
    y = idx[2]
    for shift, w in zip(SHIFTS, (w0, w1, w2, w3)):
        at = pl.multiple_of(lax.rem(y - shift + 4, 4) * 16, 16)
        out[:, pl.ds(at, 16), :] = w[...]


def assemble(*args):
    return call(assemble_body, [((32, 64, 768), BF)], 1, 4, flops=10**6, name="assemble")(*args)[0]


def conv_out_body(joined, mine, theirs, scale, w, part):
    conv = joined[...].astype(F32)
    total = mine[...] + theirs[...]
    mean = total[:, 0:1] * (1.0 / 1024)
    power = total[:, 1:2] * (1.0 / 1024) - mean * mean
    normed = (conv - mean) * lax.rsqrt(power + 1e-05) * scale[...]
    act = (normed * jax.nn.sigmoid(normed)).astype(BF)
    part[...] = dot_nt(act, w[:, 256:768])


def conv_out(*args):
    return call(
        conv_out_body, [((128, 2048), F32)], 0, 5, flops=2 * 128 * 512 * 2048, name="conv_out"
    )(*args)[0]


def mixer_out_body(idx, m0, m1, m2, m3, part, w, own, send, rows, total):
    x, c = idx[1], idx[3]
    for shift, ref in zip(SHIFTS, (m0, m1, m2, m3)):
        rows[lax.rem(x - shift + 4, 4)] = ref[...]
    act = jnp.concatenate([rows[0], rows[1], rows[2], rows[3]], axis=1)
    total[...] = part[...] + dot_nt(act, w[:, 0:256])
    own[...] = total[pl.ds(pl.multiple_of(c * 64, 64), 64), :]
    send[...] = total[pl.ds(pl.multiple_of((1 - c) * 64, 64), 64), :].astype(BF)


def mixer_out(*args):
    return call(
        mixer_out_body,
        [((64, 2048), F32), ((64, 2048), BF)],
        1,
        6,
        [pltpu.VMEM((4, 128, CH), BF), pltpu.VMEM((128, 2048), F32)],
        flops=2 * 128 * 256 * 2048,
        name="mixer_out",
    )(*args)


def ring(axis, shift):
    n = lax.axis_size(axis)
    return [(i, (i + shift) % n) for i in range(n)]


def moved(a, axis, shift):
    return lax.ppermute(a, axis, ring(axis, shift))


def swapped(a):
    return lax.ppermute(a, "tp", [(0, 1), (1, 0)])


def to_all(pieces, axes):
    return lax.all_to_all(pieces, axes, 0, 0, tiled=True)


def spread(a):
    return jnp.broadcast_to(a[None], (8, *a.shape)).reshape(8 * a.shape[0], *a.shape[1:])


def per_device(
    inputs, input_norm_scale, query_matrix, key_matrix, value_matrix, decay_down_weight,
    decay_up_weight, decay_bias_base, decay_position_offset, extra_log_decay,
    correction_down_weight, correction_up_weight, correction_rate_bias, head_norm_scale,
    starting_states, pointwise_value_weight, pointwise_gate_weight, depthwise_taps_weight,
    channel_norm_scale, mixer_output_weight, convolution_output_weight,
):
    z, x = lax.axis_index("z"), lax.axis_index("x")
    y, c = lax.axis_index("fs"), lax.axis_index("tp")
    idx = jnp.stack([z, x, y, c]).astype(jnp.int32)

    own = inputs[0]
    blocks = [own] + [moved(own, "x", s) for s in SHIFTS[1:]]
    far = [swapped(b) for b in blocks]
    marks = jnp.concatenate([decay_position_offset[0].T, extra_log_decay[0].T], axis=0)
    marks = [marks] + [moved(marks, "x", s) for s in SHIFTS[1:]]

    def heads(w):
        return w.reshape(64, 4, -1).transpose(1, 0, 2)

    wkv = to_all(
        spread(jnp.concatenate([heads(key_matrix), heads(value_matrix)], axis=2)), ("z", "x")
    ).reshape(2048, 128)
    wq = heads(query_matrix)
    late = to_all(
        spread(
            jnp.concatenate(
                [wq, wq, heads(pointwise_value_weight), heads(pointwise_gate_weight)], axis=2
            )
        ),
        ("z", "x"),
    ).reshape(2048, 384)
    quarter = jnp.concatenate(
        [
            lax.dynamic_slice_in_dim(mixer_output_weight, y * 16, 16, 1),
            lax.dynamic_slice_in_dim(convolution_output_weight, y * 16, 16, 1),
        ],
        axis=0,
    ).T
    wide = to_all(jnp.broadcast_to(quarter[None], (32, 16, 768)), ("z", "x"))

    def my_head(w, width=CH):
        return lax.dynamic_slice_in_dim(w, x * width, width, w.ndim - 1)

    def twice(w):
        return jnp.concatenate([w, w], axis=-1)

    normed, pu, pr, pq, rate = prepare(
        idx, *blocks, *far, *marks, input_norm_scale.reshape(2, 1024), decay_down_weight,
        correction_down_weight, twice(my_head(decay_up_weight)), twice(my_head(correction_up_weight)),
        twice(my_head(decay_bias_base))[None], twice(my_head(correction_rate_bias))[None],
    )
    send, resp, rs, ks, kv, pre = maps(idx, normed, wkv, pu, pr, pq, rate)
    states = to_all(send, ("z",))
    thr, rest = reads(normed, late, pq, resp, rs, ks, kv, pre)

    glu, top, bottom = gated(normed, late)
    low = lax.ppermute(bottom, "z", [(i, i + 1) for i in range(7)])
    high = lax.ppermute(top, "z", [(i + 1, i) for i in range(7)])
    sent = conv(idx, glu, low, high, my_head(depthwise_taps_weight, 128))
    convs = [sent[0]] + [moved(b, "x", s) for b, s in zip(sent[1:], SHIFTS[1:])]
    joined, stat = stats(idx, *convs)
    out_weights = assemble(idx, wide, *[moved(wide, "fs", s) for s in SHIFTS[1:]]).reshape(2048, 768)
    part = conv_out(joined, stat, swapped(stat), channel_norm_scale[None], out_weights)

    first = lax.dynamic_index_in_dim(starting_states[0], x, 1, False)
    first = jnp.concatenate([first[0], first[1]], axis=1)
    mixed = finish(idx, states, first, thr, rest, my_head(head_norm_scale)[None])
    mixes = [mixed[0]] + [moved(b, "x", s) for b, s in zip(mixed[1:], SHIFTS[1:])]
    mine, theirs = mixer_out(idx, *mixes, part, out_weights)
    return (mine + swapped(theirs).astype(F32)).astype(BF)[None]


SEQ = ("z", "x")


def solution(mesh):
    finer = Mesh(mesh.devices.reshape(8, 4, 4, 2), ("z", "x", "fs", "tp"))
    return jax.shard_map(
        per_device,
        mesh=finer,
        in_specs=(
            P("fs", SEQ, "tp"), P(), P(SEQ, "tp"), P(SEQ, "tp"), P(SEQ, "tp"), P(), P(None, "tp"),
            P("tp"), P("fs", SEQ, "tp"), P("fs", SEQ, "tp"), P(), P(None, "tp"), P("tp"), P("tp"),
            P("fs", None, "tp", None, None), P(SEQ, "tp"), P(SEQ, "tp"), P(None, "tp"), P("tp"),
            P("tp", SEQ), P("tp", SEQ),
        ),
        out_specs=P("fs", ("z", "x", "tp"), None),
        check_vma=False,
    )
```
